32 devices in a mesh: ep: 8 (over z, x), tp: 4 (over y, core).
Axes of the slice: x: 2, y: 2, z: 4, core: 2. Of those that a mesh axis runs over, the one named last changes fastest.
Arguments:
- first_micro_values: bfloat16 [8192, 2048], P('ep', 'tp'), may hold values from -6 to 6
- group_state_maps: bfloat16 [2, 8192, 1024], P(None, 'ep', 'tp'), may hold values from -6 to 6
- gate_preactivation: bfloat16 [8192, 2048], P('ep', 'tp'), may hold values from -6 to 6
- step_preactivation: float32 [8192, 32], P('ep', 'tp'), may hold values from -5.7 to 5.7
- head_step_bias: float32 [32], P('tp'), may hold values from -12 to -3
- head_log_decay: float32 [32], P('tp'), may hold values from -12 to 1
- decay_increment: float32 [8192, 32], P('ep', 'tp'), may hold values from -1.4 to 0
- head_direct_gain: float32 [32], P('tp'), may hold values from 0.1 to 1.9
- convolution_value_taps: bfloat16 [4, 2048], P(None, 'tp'), may hold values from -3 to 3
- convolution_map_taps: bfloat16 [2, 4, 1024], P(None, None, 'tp'), may hold values from -3 to 3
- grouped_norm_gain: float32 [2048], P('tp'), may hold values from 0.1 to 1.9
- second_micro_tokens: bfloat16 [8192, 2048], P(('ep', 'tp')), may hold values from -6 to 6
- expert_norm_gain: float32 [2048], replicated, may hold values from 0.1 to 1.9
- routes: int32 [8192, 2], P(('ep', 'tp')), may hold values from 0 to 7, all different within a row; in each aligned block of 256 rows (0 to 255, 256 to 511, ...) at most 96 rows name the same one
- visit_weight: float32 [8192, 2], P(('ep', 'tp')), may hold values from 0.1 to 1
- gate_weight_table: bfloat16 [8, 2048, 1024], P('ep', None, 'tp'), may hold values from -0.125 to 0.125
- up_weight_table: bfloat16 [8, 2048, 1024], P('ep', None, 'tp'), may hold values from -0.125 to 0.125
- down_weight_table: bfloat16 [8, 2048, 1024], P('ep', None, 'tp'), may hold values from -0.1875 to 0.1875
Outputs:
- mixer_gated_output: bfloat16 [8192, 2048], P('ep', 'tp')
- routed_out: bfloat16 [8192, 2048], P(('ep', 'tp'))
The draws below stay inside these ranges and needn't reach their ends.
Inputs may be any that keep to these rules, and one draw needn't show every extreme that they name: `routes`: A row names 2 different experts. In each aligned block of 256 rows (the rows of one device), no expert is named by more than 96 rows, a bound that some block reaches.
All inputs are finite; a program needn't handle non-finite values.
Results may differ from the reference program's by a relative error of at most 0.0071.
Values may be sent and summed in bfloat16 or wider, within the bound.
A program may use at most 128 MiB of HBM per device.

```python
import math
import jax
import jax.numpy as jnp
import numpy as np
from jax import lax

D = 2048
FF = 1024
HEADS = 32
HEADDIM = 64
GROUPS = 8
NSTATE = 128
CONV = 4
BLOCK = 128
TOPK = 2
TOK_DEV = 256
SEQ_DEV = 1024
SEQ = 8192
TOKENS = 8192
EXPERTS = 8
CAP = 96
INNER = 2048
N_EP = 8
N_TP = 4


def fast_heads(key):
    fast_share = 0.5
    return jax.random.uniform(jax.random.fold_in(key, 71), (HEADS,), jnp.float32) < fast_share


def draw_head_step_bias(key, part):
    fast_mask = fast_heads(key)
    jitter = jax.random.uniform(jax.random.fold_in(key, 72), (HEADS,), jnp.float32, -0.3, 0.3)
    slow_level = jnp.log(0.25 / jnp.sqrt(jnp.float32(SEQ)))
    return jnp.where(fast_mask, jnp.log(jnp.float32(0.02)), slow_level) + jitter


def draw_head_log_decay(key, part):
    fast_mask = fast_heads(key)
    jitter = jax.random.uniform(jax.random.fold_in(key, 73), (HEADS,), jnp.float32, -0.3, 0.3)
    slow_level = jnp.log(2.0 / jnp.sqrt(jnp.float32(SEQ)))
    return jnp.where(fast_mask, jnp.log(jnp.float32(1.5)), slow_level) + jitter


def draw_step_preactivation(key, part):
    noise_part = jnp.clip(jax.random.normal(jax.random.fold_in(key, 81), (SEQ, HEADS), jnp.float32), -5.0, 5.0)
    offsets = jax.random.uniform(jax.random.fold_in(key, 82), (SEQ // SEQ_DEV, HEADS), jnp.float32, -0.7, 0.7)
    return noise_part + jnp.repeat(offsets, SEQ_DEV, axis=0)


def draw_decay_increment(key, part):
    position_list = jax.random.randint(jax.random.fold_in(key, 91), (2, HEADS), 0, SEQ, dtype=jnp.int32)
    error_terms = jnp.log(jax.random.uniform(jax.random.fold_in(key, 92), (2, HEADS), jnp.float32, 0.5, 0.8))
    sequence_position_index = jnp.arange(SEQ, dtype=jnp.int32)[:, None]
    summed_total = jnp.zeros((SEQ, HEADS), jnp.float32)
    for spike_index in range(2):
        summed_total = summed_total + jnp.where(sequence_position_index == position_list[spike_index][None, :], error_terms[spike_index][None, :], 0.0)
    return summed_total


def shard_levels(own_key, dims, cuts, smallest, top_value):
    loudness, own = 1.0, jax.random.fold_in(own_key, 6)
    for axis_at, parts in cuts:
        steps = jnp.exp(jax.random.uniform(jax.random.fold_in(own, axis_at), (parts,), jnp.float32, smallest / len(cuts), top_value / len(cuts)))
        loudness = loudness * jnp.repeat(steps, dims[axis_at] // parts).reshape([-1 if axis == axis_at else 1 for axis in range(len(dims))])
    return loudness


def deal_out(key, own, number, rows, number_of, top, most, lean):
    order = jax.random.permutation(key, number_of)
    crowded, common = portions_of(number_of, rows * top, most, lean, True), portions_of(number_of, rows * top, most, lean, False)
    places = jnp.arange(number_of)

    def named(sizes, offset_by):
        used = int((sizes > 0).sum())
        fixed = max(1, used // 4)
        shifted = fixed + (places - fixed + offset_by * (used - fixed)) % max(1, number_of - fixed)
        return jnp.zeros((number_of,), jnp.int32).at[order[jnp.where(places < fixed, places, shifted)]].set(jnp.asarray(sizes, jnp.int32))

    sizes = jnp.where(number % 4 == 0, named(crowded, number // 4), named(common, number - number // 4 - 1))
    mixed = jax.random.permutation(jax.random.fold_in(own, 3), number_of)
    giver, sink = mixed[0:number_of // 2 * 2:2], mixed[1:number_of // 2 * 2:2]
    slack = jnp.minimum(sizes[giver] - 1, most - sizes[sink]) // 2
    slack = jnp.where((giver == order[0]) | (sink == order[0]) | (sizes[sink] == 0), 0, jnp.maximum(slack, 0))
    shifted = jax.random.randint(jax.random.fold_in(own, 4), (number_of // 2,), 0, 1 << 20) % (slack + 1)
    sizes = sizes.at[giver].add(-shifted).at[sink].add(shifted)
    labels = jnp.searchsorted(jnp.cumsum(sizes), jnp.arange(rows * top), side="right").astype(jnp.int32)
    table = labels.reshape(top, rows).T
    table = table[jax.random.permutation(jax.random.fold_in(own, 1), rows)]
    offset_by = jax.random.randint(jax.random.fold_in(own, 2), (rows, 1), 0, top)
    return jnp.take_along_axis(table, (jnp.arange(top)[None, :] + offset_by) % top, axis=1)


def portions_of(number_of, total, bound, skew, full):
    portions = [(1 << 20) // math.isqrt(rank ** skew) + 1 for rank in range(1, number_of + 1)]
    largest = bound if full else min(bound, max(-(-total // number_of), total * portions[0] // sum(portions)))
    least = 1 if total - largest >= number_of - 1 else 0
    counts, spare = [largest] + [least] * (number_of - 1), total - largest - least * (number_of - 1)
    while spare > 0:
        movable = [i for i in range(1, number_of) if counts[i] < largest] or [i for i in range(1, number_of) if counts[i] < bound]
        whole, budget = sum([portions[i] for i in movable]), spare
        for i in movable:
            extra = min(bound - counts[i], max(1, budget * portions[i] // whole), spare)
            counts[i] = counts[i] + extra
            spare = spare - extra
    return np.array(counts)


def bell_draw(own_key, dims, deviation, most, split=(), kind=jnp.bfloat16):
    values = jax.random.normal(own_key, dims, jnp.float32) * deviation
    if len(split) > 0:
        values = shard_levels(own_key, dims, split, -0.22, 0.18) * values
    return jnp.clip(values, min=-most, max=most).astype(kind)


def setup_inputs(seed: int = 0) -> dict:
    key_of = jax.random.split(jax.random.key(seed), 19)
    first_micro_values = bell_draw(key_of[0], (SEQ, INNER), 1.0, 6.0, ((0, 8), (1, 4)))
    group_state_maps = bell_draw(key_of[1], (2, SEQ, GROUPS * NSTATE), 1.0, 6.0, ((1, 8), (2, 4)))
    gate_preactivation = bell_draw(key_of[2], (SEQ, INNER), 1.0, 6.0, ((0, 8), (1, 4)))
    step_preactivation = draw_step_preactivation(jax.random.fold_in(key_of[18], 71), 0)
    head_step_bias = draw_head_step_bias(jax.random.fold_in(key_of[18], 71), 0)
    head_log_decay = draw_head_log_decay(jax.random.fold_in(key_of[18], 71), 0)
    decay_increment = draw_decay_increment(jax.random.fold_in(key_of[18], 71), 0)
    head_direct_gain = jnp.clip(1.0 + 0.18 * jax.random.normal(key_of[7], (HEADS,), jnp.float32), 0.1, 1.9)
    convolution_value_taps = bell_draw(key_of[8], (CONV, INNER), CONV ** -0.5, 3.0, ((1, 4),))
    convolution_map_taps = bell_draw(key_of[9], (2, CONV, GROUPS * NSTATE), CONV ** -0.5, 3.0, ((2, 4),))
    grouped_norm_gain = jnp.clip(1.0 + 0.18 * jax.random.normal(key_of[10], (INNER,), jnp.float32), 0.1, 1.9)
    second_micro_tokens = bell_draw(key_of[11], (TOKENS, D), 1.0, 6.0, ((0, 32),))
    expert_norm_gain = jnp.clip(1.0 + 0.18 * jax.random.normal(key_of[12], (D,), jnp.float32), 0.1, 1.9)
    routes_keys = jax.random.split(jax.random.fold_in(key_of[13], 1), TOKENS // TOK_DEV)
    routes_turns = jax.random.permutation(jax.random.fold_in(key_of[13], 3), TOKENS // TOK_DEV)
    routes = jax.vmap(lambda own, number: deal_out(jax.random.fold_in(key_of[13], 2), own, number, TOK_DEV, EXPERTS, TOPK, CAP, 0))(routes_keys, routes_turns).reshape((TOKENS, TOPK))
    visit_weight = jnp.clip(0.1 + 0.9 * jax.random.uniform(key_of[14], (TOKENS, TOPK), jnp.float32) ** shard_levels(key_of[14], (TOKENS, TOPK), ((0, 32),), -0.2, 0.2), 0.1, 1.0)
    gate_weight_table = bell_draw(key_of[15], (EXPERTS, D, FF), D ** -0.5, 0.125, ((0, 8), (2, 4)))
    up_weight_table = bell_draw(key_of[16], (EXPERTS, D, FF), D ** -0.5, 0.125, ((0, 8), (2, 4)))
    down_weight_table = bell_draw(key_of[17], (EXPERTS, D, FF), FF ** -0.5, 0.1875, ((0, 8), (2, 4)))
    return dict(first_micro_values=first_micro_values, group_state_maps=group_state_maps, gate_preactivation=gate_preactivation, step_preactivation=step_preactivation, head_step_bias=head_step_bias, head_log_decay=head_log_decay, decay_increment=decay_increment, head_direct_gain=head_direct_gain, convolution_value_taps=convolution_value_taps, convolution_map_taps=convolution_map_taps, grouped_norm_gain=grouped_norm_gain, second_micro_tokens=second_micro_tokens, expert_norm_gain=expert_norm_gain, routes=routes, visit_weight=visit_weight, gate_weight_table=gate_weight_table, up_weight_table=up_weight_table, down_weight_table=down_weight_table)


HIGHEST = lax.Precision.HIGHEST
EPSILON = 1e-05

def causal_conv(values, weights):
    length = values.shape[0]
    kernel = weights.shape[0]
    padded = jnp.pad(values.astype(jnp.float32), ((kernel - 1, 0), (0, 0)))
    summed_total = jnp.zeros(values.shape, jnp.float32)
    for offset in range(kernel):
        summed_total = summed_total + weights[offset].astype(jnp.float32) * padded[offset:offset + length]
    return jax.nn.silu(summed_total)

def mixer_baseline(first_micro_values, group_state_maps, gate_preactivation, step_preactivation, head_step_bias, head_log_decay, decay_increment, head_direct_gain, convolution_value_taps, convolution_map_taps, grouped_norm_gain):
    length, channels = first_micro_values.shape
    head_count = step_preactivation.shape[1]
    per_group = head_count // GROUPS
    blocks = length // BLOCK
    conv_out = causal_conv(first_micro_values, convolution_value_taps)
    in_maps = causal_conv(group_state_maps[0], convolution_map_taps[0])
    out_maps = causal_conv(group_state_maps[1], convolution_map_taps[1])
    step_length = jax.nn.softplus(step_preactivation + head_step_bias)
    decay_logarithm = -jnp.exp(head_log_decay) * step_length + decay_increment
    head_values = conv_out.reshape(blocks, BLOCK, GROUPS, per_group, HEADDIM)
    scaled_values = head_values * step_length.reshape(blocks, BLOCK, GROUPS, per_group)[..., None]
    in_blocks = in_maps.reshape(blocks, BLOCK, GROUPS, NSTATE)
    out_blocks = out_maps.reshape(blocks, BLOCK, GROUPS, NSTATE)
    running = jnp.cumsum(decay_logarithm.reshape(blocks, BLOCK, GROUPS, per_group), axis=1)
    causal = jnp.tril(jnp.ones((BLOCK, BLOCK), dtype=bool))

    def one_block(carry_state, inputs):
        value_block, in_block, out_block, running_block = inputs
        scores = jnp.einsum('lgn,sgn->gls', out_block, in_block, precision=HIGHEST)
        ordered = jnp.moveaxis(running_block, 0, -1)
        between = jnp.exp(jnp.where(causal, ordered[..., :, None] - ordered[..., None, :], -jnp.inf))
        inside = jnp.einsum('grls,sgrp->lgrp', scores[:, None] * between, value_block, precision=HIGHEST)
        carried = jnp.einsum('lgn,grpn->lgrp', out_block, carry_state, precision=HIGHEST)
        carried = carried * jnp.exp(running_block)[..., None]
        to_end = jnp.exp(running_block[-1][None] - running_block)
        block_states = jnp.einsum('lgn,lgr,lgrp->grpn', in_block, to_end, value_block, precision=HIGHEST)
        next_state = carry_state * jnp.exp(running_block[-1])[..., None, None] + block_states
        return (next_state, inside + carried)
    zero_state = jnp.zeros((GROUPS, per_group, HEADDIM, NSTATE), jnp.float32)
    unused, outputs = lax.scan(one_block, zero_state, (scaled_values, in_blocks, out_blocks, running))
    mixed_out = outputs + head_values * head_direct_gain.reshape(GROUPS, per_group)[:, :, None]
    gated_out = mixed_out.reshape(length, channels) * jax.nn.silu(gate_preactivation.astype(jnp.float32))
    grouped = gated_out.reshape(length, GROUPS, channels // GROUPS)
    normed = grouped * lax.rsqrt(lax.optimization_barrier(jnp.mean(grouped * grouped, axis=-1, keepdims=True)) + EPSILON)
    return (normed.reshape(length, channels) * grouped_norm_gain).astype(jnp.bfloat16)

def routed_reference(second_micro_tokens, expert_norm_gain, routes, visit_weight, gate_weight_table, up_weight_table, down_weight_table):
    tokens, feature_count = second_micro_tokens.shape
    fanout = routes.shape[1]
    experts = gate_weight_table.shape[0]
    values = second_micro_tokens.astype(jnp.float32)
    centered = values - lax.optimization_barrier(jnp.mean(values, axis=1, keepdims=True))
    normed = centered * lax.rsqrt(lax.optimization_barrier(jnp.mean(centered * centered, axis=1, keepdims=True)) + EPSILON)
    normed = (normed * expert_norm_gain).astype(jnp.bfloat16)
    flat_routes = routes.reshape(-1)
    one_hot = (flat_routes[:, None] == jnp.arange(experts, dtype=jnp.int32)[None, :]).astype(jnp.int32)
    slot_index = lax.optimization_barrier(jnp.sum(jnp.cumsum(one_hot, axis=0) * one_hot, axis=1)) - 1
    limit = N_EP * N_TP * CAP
    owners = jnp.arange(tokens * fanout, dtype=jnp.int32) // fanout
    table = jnp.full((experts, limit), tokens, jnp.int32).at[flat_routes, slot_index].set(owners)
    scales = jnp.zeros((experts, limit), jnp.float32).at[flat_routes, slot_index].set(visit_weight.reshape(-1))
    padded = jnp.concatenate([normed, jnp.zeros((1, feature_count), jnp.bfloat16)], axis=0)

    def one_expert(running_sum, inputs):
        row_index, row_scale, gate_piece, up_piece, down_piece = inputs
        routed_rows = padded[row_index]
        activated = jax.nn.silu(jnp.dot(routed_rows, gate_piece, preferred_element_type=jnp.float32))
        hidden = (activated * jnp.dot(routed_rows, up_piece, preferred_element_type=jnp.float32)).astype(jnp.bfloat16)
        result = lax.dot_general(hidden, down_piece, (((1,), (1,)), ((), ())), preferred_element_type=jnp.float32).astype(jnp.bfloat16)
        return (running_sum.at[row_index].add(result.astype(jnp.float32) * row_scale[:, None]), None)
    zero_sum = jnp.zeros((tokens + 1, feature_count), jnp.float32)
    summed_total, unused = lax.scan(one_expert, zero_sum, (table, scales, gate_weight_table, up_weight_table, down_weight_table))
    return summed_total[:tokens].astype(jnp.bfloat16)

def reference(first_micro_values, group_state_maps, gate_preactivation, step_preactivation, head_step_bias, head_log_decay, decay_increment, head_direct_gain, convolution_value_taps, convolution_map_taps, grouped_norm_gain, second_micro_tokens, expert_norm_gain, routes, visit_weight, gate_weight_table, up_weight_table, down_weight_table):
    mixer_gated_output = mixer_baseline(first_micro_values, group_state_maps, gate_preactivation, step_preactivation, head_step_bias, head_log_decay, decay_increment, head_direct_gain, convolution_value_taps, convolution_map_taps, grouped_norm_gain)
    routed_out = routed_reference(second_micro_tokens, expert_norm_gain, routes, visit_weight, gate_weight_table, up_weight_table, down_weight_table)
    return (mixer_gated_output, routed_out)
```

```python
import functools

import jax
import jax.numpy as jnp
from jax import lax
from jax.experimental import pallas as pl
from jax.experimental.pallas import tpu as pltpu
from jax.sharding import PartitionSpec as P

HEADDIM = 64
NSTATE = 128
BLOCK = 128
LANES = 128
HALO = 8
RETURN_CHUNKS = 2

HIGHEST = lax.Precision.HIGHEST
EPSILON = 1e-05
F32 = jnp.float32
BF16 = jnp.bfloat16


def cost(flops, bytes_accessed):
    return pl.CostEstimate(flops=int(flops), bytes_accessed=int(bytes_accessed), transcendentals=0)


def params(*semantics):
    return pltpu.CompilerParams(dimension_semantics=semantics, vmem_limit_bytes=48 * 1024 * 1024)


def silu(x):
    return x / (1.0 + jnp.exp(-x))


def dot(a, b, dims=(((1,), (0,)), ((), ()))):
    return lax.dot_general(a, b, dims, preferred_element_type=F32)


def spread(columns, pair):
    rows = columns.shape[0]
    lane = lax.broadcasted_iota(jnp.int32, (rows, LANES), 1)
    first = jnp.broadcast_to(columns[:, 2 * pair : 2 * pair + 1], (rows, LANES))
    second = jnp.broadcast_to(columns[:, 2 * pair + 1 : 2 * pair + 2], (rows, LANES))
    return jnp.where(lane < HEADDIM, first, second)


def mixer_local_kernel(
    values_ref,
    maps_ref,
    before_ref,
    step_ref,
    increment_ref,
    bias_ref,
    rate_ref,
    direct_ref,
    value_taps_ref,
    map_taps_ref,
    y_ref,
    out_maps_ref,
    prefix_ref,
    end_ref,
    extended,
    state,
    total,
):
    block = pl.program_id(0)
    channels = values_ref.shape[1]
    width = maps_ref.shape[2]
    groups = width // NSTATE
    heads = step_ref.shape[1]
    per_group = heads // groups
    group_lanes = per_group * HEADDIM
    taps = value_taps_ref.shape[0]

    @pl.when(block == 0)
    def _():
        extended[0:HALO, :] = before_ref[...].astype(F32)
        state[...] = jnp.zeros_like(state)
        total[...] = jnp.zeros_like(total)

    extended[HALO:, 0:channels] = values_ref[...].astype(F32)
    extended[HALO:, channels : channels + width] = maps_ref[0].astype(F32)
    extended[HALO:, channels + width :] = maps_ref[1].astype(F32)

    def conv(start, stop, weights):
        summed = jnp.zeros((BLOCK, stop - start), F32)
        for j in range(taps):
            at = HALO - (taps - 1) + j
            summed = summed + weights[j : j + 1, :] * extended[at : at + BLOCK, start:stop]
        return silu(summed)

    step = jax.nn.softplus(step_ref[...] + bias_ref[...])
    log_decay = step * rate_ref[...] + increment_ref[...]
    row = lax.broadcasted_iota(jnp.int32, (BLOCK, BLOCK), 0)
    column = lax.broadcasted_iota(jnp.int32, (BLOCK, BLOCK), 1)
    causal = row >= column
    running = lax.dot_general(
        causal.astype(F32),
        log_decay,
        (((1,), (0,)), ((), ())),
        precision=HIGHEST,
        preferred_element_type=F32,
    )
    running_rows = jnp.transpose(running)
    block_total = running[BLOCK - 1 : BLOCK, :]
    decay_in = jnp.exp(running)
    to_end = jnp.exp(block_total - running)
    prefix_ref[...] = jnp.exp(running + total[...])
    total[...] = total[...] + block_total
    block_decay = jnp.exp(block_total)

    for g in range(groups):
        in_map = conv(
            channels + g * NSTATE, channels + (g + 1) * NSTATE, map_taps_ref[0, :, g * NSTATE : (g + 1) * NSTATE].astype(F32)
        ).astype(BF16)
        out_map = conv(
            channels + width + g * NSTATE,
            channels + width + (g + 1) * NSTATE,
            map_taps_ref[1, :, g * NSTATE : (g + 1) * NSTATE].astype(F32),
        ).astype(BF16)
        out_maps_ref[:, g * NSTATE : (g + 1) * NSTATE] = out_map
        scores = dot(out_map, in_map, (((1,), (1,)), ((), ())))
        scores = jnp.where(causal, scores, 0.0)
        for pair in range(per_group // 2):
            first = g * (per_group // 2) + pair
            lanes = slice(first * LANES, (first + 1) * LANES)
            inner = slice(pair * LANES, (pair + 1) * LANES)
            x = conv(lanes.start, lanes.stop, value_taps_ref[:, lanes].astype(F32))
            scaled = x * spread(step, first)
            scaled_low = scaled.astype(BF16)
            parts = []
            for h in (2 * first, 2 * first + 1):
                gap = running[:, h : h + 1] - running_rows[h : h + 1, :]
                weights = scores * jnp.exp(jnp.minimum(gap, 0.0))
                parts.append(dot(weights.astype(BF16), scaled_low))
            lane = lax.broadcasted_iota(jnp.int32, (BLOCK, LANES), 1)
            inside = jnp.where(lane < HEADDIM, parts[0], parts[1])
            entering = state[g, :, inner]
            carried = dot(out_map, entering.astype(BF16)) * spread(decay_in, first)
            y_ref[:, lanes] = inside + carried + x * spread(direct_ref[...], first)
            ending = (scaled * spread(to_end, first)).astype(BF16)
            added = dot(in_map, ending, (((0,), (0,)), ((), ())))
            state[g, :, inner] = entering * spread(block_decay, first) + added

    extended[0:HALO, :] = extended[BLOCK : BLOCK + HALO, :]

    @pl.when(block == pl.num_programs(0) - 1)
    def _():
        end_ref[0 : groups * NSTATE, :] = state[...].reshape(groups * NSTATE, group_lanes)
        total_decay = jnp.exp(total[...])
        end_ref[groups * NSTATE :, :] = jnp.zeros((8, group_lanes), F32)
        for g in range(groups):
            for pair in range(per_group // 2):
                inner = slice(pair * LANES, (pair + 1) * LANES)
                at = groups * NSTATE + g
                end_ref[at : at + 1, inner] = spread(total_decay, g * (per_group // 2) + pair)


def mixer_finish_kernel(y_ref, out_maps_ref, prefix_ref, incoming_ref, gate_ref, gain_ref, out_ref):
    heads = prefix_ref.shape[1]
    groups = out_maps_ref.shape[1] // NSTATE
    per_group = heads // groups
    prefix = prefix_ref[...]
    for g in range(groups):
        out_map = out_maps_ref[:, g * NSTATE : (g + 1) * NSTATE]
        parts = []
        squares = 0.0
        for pair in range(per_group // 2):
            first = g * (per_group // 2) + pair
            lanes = slice(first * LANES, (first + 1) * LANES)
            incoming = incoming_ref[
                g * NSTATE : (g + 1) * NSTATE, pair * LANES : (pair + 1) * LANES
            ]
            y = y_ref[:, lanes] + dot(out_map, incoming.astype(BF16)) * spread(prefix, first)
            gated = y * silu(gate_ref[:, lanes].astype(F32))
            squares = squares + jnp.sum(gated * gated, axis=1, keepdims=True)
            parts.append((lanes, gated))
        scale = lax.rsqrt(squares / (per_group * HEADDIM) + EPSILON)
        for lanes, gated in parts:
            out_ref[:, lanes] = (gated * scale * gain_ref[:, lanes]).astype(BF16)


def dispatch_kernel(tokens_ref, gain_ref, routes_ref, rows_ref, target_ref, *, capacity):
    tokens = tokens_ref.shape[0]
    rows = rows_ref.shape[0]
    values = tokens_ref[...].astype(F32)
    centered = values - jnp.mean(values, axis=1, keepdims=True)
    variance = jnp.mean(centered * centered, axis=1, keepdims=True)
    normed = (centered * lax.rsqrt(variance + EPSILON) * gain_ref[...]).astype(BF16)
    routes = routes_ref[...]
    fanout = routes.shape[1]
    experts = lax.broadcasted_iota(jnp.int32, (tokens, LANES), 1)
    visits = jnp.zeros((tokens, LANES), F32)
    for k in range(fanout):
        visits = visits + (experts == routes[:, k : k + 1]).astype(F32)
    row = lax.broadcasted_iota(jnp.int32, (tokens, tokens), 0)
    column = lax.broadcasted_iota(jnp.int32, (tokens, tokens), 1)
    slots = dot((row > column).astype(F32).astype(BF16), visits.astype(BF16)).astype(jnp.int32)
    slots = slots + experts * capacity
    places = lax.broadcasted_iota(jnp.int32, (tokens, rows), 1)
    chosen = jnp.zeros((tokens, rows), F32)
    for k in range(fanout):
        target = jnp.sum(
            jnp.where(experts == routes[:, k : k + 1], slots.astype(F32), 0.0), axis=1, keepdims=True
        ).astype(jnp.int32)
        target_ref[:, k : k + 1] = target
        chosen = chosen + (places == target).astype(F32)
    rows_ref[...] = dot(chosen.astype(BF16), normed, (((0,), (0,)), ((), ()))).astype(BF16)


def combine_kernel(returned_ref, target_ref, weight_ref, out_ref):
    tokens = target_ref.shape[0]
    rows = returned_ref.shape[0]
    places = lax.broadcasted_iota(jnp.int32, (tokens, rows), 1)
    table = jnp.zeros((tokens, rows), F32)
    for k in range(target_ref.shape[1]):
        table = table + jnp.where(places == target_ref[:, k : k + 1], weight_ref[:, k : k + 1], 0.0)
    high = table.astype(BF16)
    low = (table - high.astype(F32)).astype(BF16)
    returned = returned_ref[...]
    out_ref[...] = (dot(high, returned) + dot(low, returned)).astype(BF16)


def hidden_kernel(rows_ref, gate_ref, up_ref, hidden_ref):
    rows = rows_ref[...]
    activated = silu(dot(rows, gate_ref[0]))
    hidden_ref[...] = (activated * dot(rows, up_ref[0])).astype(BF16)


def down_kernel(*refs):
    count = (len(refs) - 1) // 2
    total = 0.0
    for hidden_ref, down_ref in zip(refs[:count], refs[count : 2 * count]):
        total = total + dot(hidden_ref[...], down_ref[0], (((1,), (1,)), ((), ())))
    refs[-1][...] = total.astype(BF16)


def whole(shape):
    return pl.BlockSpec(shape, lambda *_: (0,) * len(shape))


def shifted(block, axis, distance):
    devices = range(lax.axis_size(axis))
    route = [(i - distance, i) for i in devices if i - distance in devices]
    return lax.ppermute(block, axis, route)


def flipped(block, axis, bit):
    return lax.ppermute(block, axis, [(i, i ^ bit) for i in range(lax.axis_size(axis))])


def all_shards(block, axis):
    pieces = [block]
    bit = lax.axis_size(axis) // 2
    while bit:
        pieces = pieces + [flipped(piece, axis, bit) for piece in pieces]
        bit //= 2
    return pieces


def mixer_local(
    values,
    maps,
    step_preactivation,
    step_bias,
    log_rate,
    increment,
    direct,
    value_taps,
    map_taps,
):
    length, channels = values.shape
    heads = step_preactivation.shape[1]
    width = maps.shape[2]
    groups = width // NSTATE
    group_lanes = channels // groups
    tail_rows = jnp.concatenate(
        [values[length - HALO :], maps[0, length - HALO :], maps[1, length - HALO :]], axis=1
    )
    before = shifted(tail_rows, "ep", 1)
    taps = value_taps.shape[0]
    return pl.pallas_call(
        mixer_local_kernel,
        grid=(length // BLOCK,),
        in_specs=[
            pl.BlockSpec((BLOCK, channels), lambda i: (i, 0)),
            pl.BlockSpec((2, BLOCK, width), lambda i: (0, i, 0)),
            whole((HALO, channels + 2 * width)),
            pl.BlockSpec((BLOCK, heads), lambda i: (i, 0)),
            pl.BlockSpec((BLOCK, heads), lambda i: (i, 0)),
            whole((1, heads)),
            whole((1, heads)),
            whole((1, heads)),
            whole((taps, channels)),
            whole((2, taps, width)),
        ],
        out_specs=[
            pl.BlockSpec((BLOCK, channels), lambda i: (i, 0)),
            pl.BlockSpec((BLOCK, width), lambda i: (i, 0)),
            pl.BlockSpec((BLOCK, heads), lambda i: (i, 0)),
            whole((groups * NSTATE + 8, group_lanes)),
        ],
        out_shape=[
            jax.ShapeDtypeStruct((length, channels), F32),
            jax.ShapeDtypeStruct((length, width), BF16),
            jax.ShapeDtypeStruct((length, heads), F32),
            jax.ShapeDtypeStruct((groups * NSTATE + 8, group_lanes), F32),
        ],
        scratch_shapes=[
            pltpu.VMEM((BLOCK + HALO, channels + 2 * width), F32),
            pltpu.VMEM((groups, NSTATE, group_lanes), F32),
            pltpu.VMEM((1, heads), F32),
        ],
        compiler_params=params("arbitrary"),
        cost_estimate=cost(15e9, 8e6),
        name="mixer_local",
    )(
        values,
        maps,
        before,
        step_preactivation,
        increment,
        step_bias[None],
        -jnp.exp(log_rate)[None],
        direct[None],
        value_taps,
        map_taps,
    )


def incoming_state(end, groups):
    split = groups * NSTATE

    def combined(earlier, later):
        decay = later[split : split + groups]
        states = later[:split].reshape(groups, NSTATE, -1) + decay[:, None, :] * earlier[
            :split
        ].reshape(groups, NSTATE, -1)
        return jnp.concatenate(
            [states.reshape(split, -1), later[split:] * earlier[split:]], axis=0
        )

    carried = shifted(end, "ep", 1)
    distance = 1
    while distance < lax.axis_size("ep") - 1:
        carried = combined(shifted(carried, "ep", distance), carried)
        distance *= 2
    return carried


def mixer_finish(y, out_maps, prefix, incoming, gate, gain):
    length, channels = y.shape
    tile = min(256, length)
    width = out_maps.shape[1]
    return pl.pallas_call(
        mixer_finish_kernel,
        grid=(length // tile,),
        in_specs=[
            pl.BlockSpec((tile, channels), lambda i: (i, 0)),
            pl.BlockSpec((tile, width), lambda i: (i, 0)),
            pl.BlockSpec((tile, prefix.shape[1]), lambda i: (i, 0)),
            whole(incoming.shape),
            pl.BlockSpec((tile, channels), lambda i: (i, 0)),
            whole((1, channels)),
        ],
        out_specs=pl.BlockSpec((tile, channels), lambda i: (i, 0)),
        out_shape=jax.ShapeDtypeStruct((length, channels), BF16),
        compiler_params=params("arbitrary"),
        cost_estimate=cost(4e9, 8e6),
        name="mixer_finish",
    )(y, out_maps, prefix, incoming, gate, gain[None])


def dispatched(tokens, gain, routes, rows, capacity):
    count, features = tokens.shape
    return pl.pallas_call(
        functools.partial(dispatch_kernel, capacity=capacity),
        out_shape=[
            jax.ShapeDtypeStruct((rows, features), BF16),
            jax.ShapeDtypeStruct(routes.shape, jnp.int32),
        ],
        compiler_params=params(),
        cost_estimate=cost(2e9, 5e6),
        name="dispatch",
    )(tokens, gain[None], routes)


def hidden_units(rows, gate, up):
    count, features = rows.shape
    units = gate.shape[2]
    tile = count // 3 if count % 48 == 0 else count
    return pl.pallas_call(
        hidden_kernel,
        grid=(count // tile,),
        in_specs=[
            pl.BlockSpec((tile, features), lambda i: (i, 0)),
            whole(gate.shape),
            whole(up.shape),
        ],
        out_specs=pl.BlockSpec((tile, units), lambda i: (i, 0)),
        out_shape=jax.ShapeDtypeStruct((count, units), BF16),
        compiler_params=params("arbitrary"),
        cost_estimate=cost(2 * count * features * units * 2, 5e6),
        name="hidden",
    )(rows, gate, up)


def projected(hiddens, downs, chunk, chunks):
    count, units = hiddens[0].shape
    features = downs[0].shape[1] // chunks
    tile = min(512, features)
    steps = features // tile
    return pl.pallas_call(
        down_kernel,
        grid=(steps,),
        in_specs=[whole(h.shape) for h in hiddens]
        + [pl.BlockSpec((1, tile, units), lambda i: (0, i + chunk * steps, 0)) for d in downs],
        out_specs=pl.BlockSpec((count, tile), lambda i: (0, i)),
        out_shape=jax.ShapeDtypeStruct((count, features), BF16),
        compiler_params=params("arbitrary"),
        cost_estimate=cost(2 * count * features * units * len(downs), 5e6),
        name="down",
    )(*hiddens, *downs)


def combined_rows(returned, target, weight):
    rows, features = returned.shape
    tile = min(512, features)
    return pl.pallas_call(
        combine_kernel,
        grid=(features // tile,),
        in_specs=[
            pl.BlockSpec((rows, tile), lambda i: (0, i)),
            whole(target.shape),
            whole(weight.shape),
        ],
        out_specs=pl.BlockSpec((target.shape[0], tile), lambda i: (0, i)),
        out_shape=jax.ShapeDtypeStruct((target.shape[0], features), BF16),
        compiler_params=params("arbitrary"),
        cost_estimate=cost(2e9, 4e6),
        name="combine",
    )(returned, target, weight)


def exchanged(rows, experts):
    count, features = rows.shape
    swapped = lax.all_to_all(
        rows.reshape(experts, count // experts, features),
        "ep",
        split_axis=0,
        concat_axis=0,
        tiled=True,
    )
    return swapped.reshape(count, features)


def body(
    first_micro_values,
    group_state_maps,
    gate_preactivation,
    step_preactivation,
    head_step_bias,
    head_log_decay,
    decay_increment,
    head_direct_gain,
    convolution_value_taps,
    convolution_map_taps,
    grouped_norm_gain,
    second_micro_tokens,
    expert_norm_gain,
    routes,
    visit_weight,
    gate_weight_table,
    up_weight_table,
    down_weight_table,
):
    tokens = second_micro_tokens.shape[0]
    experts = lax.axis_size("ep")
    capacity = max(2, 3 * tokens * routes.shape[1] // (2 * experts))
    gates = all_shards(gate_weight_table, "tp")
    ups = all_shards(up_weight_table, "tp")
    downs = all_shards(down_weight_table, "tp")
    outgoing, target = dispatched(
        second_micro_tokens, expert_norm_gain, routes, experts * capacity, capacity
    )
    arrived = exchanged(outgoing, experts)
    y, out_maps, prefix, end = mixer_local(
        first_micro_values,
        group_state_maps,
        step_preactivation,
        head_step_bias,
        head_log_decay,
        decay_increment,
        head_direct_gain,
        convolution_value_taps,
        convolution_map_taps,
    )
    incoming = incoming_state(end, group_state_maps.shape[2] // NSTATE)
    mixer_out = mixer_finish(y, out_maps, prefix, incoming, gate_preactivation, grouped_norm_gain)
    hiddens = [hidden_units(arrived, g, u) for g, u in zip(gates, ups)]
    pieces = []
    for chunk in range(RETURN_CHUNKS):
        results = projected(hiddens, downs, chunk, RETURN_CHUNKS)
        returned = exchanged(results, experts)
        pieces.append(combined_rows(returned, target, visit_weight))
    return (mixer_out, jnp.concatenate(pieces, axis=1))


def solution(mesh):
    placed = (
        P("ep", "tp"),
        P(None, "ep", "tp"),
        P("ep", "tp"),
        P("ep", "tp"),
        P("tp"),
        P("tp"),
        P("ep", "tp"),
        P("tp"),
        P(None, "tp"),
        P(None, None, "tp"),
        P("tp"),
        P(("ep", "tp"), None),
        P(),
        P(("ep", "tp"), None),
        P(("ep", "tp"), None),
        P("ep", None, "tp"),
        P("ep", None, "tp"),
        P("ep", None, "tp"),
    )
    return jax.shard_map(
        body,
        mesh=mesh,
        in_specs=placed,
        out_specs=(P("ep", "tp"), P(("ep", "tp"), None)),
        check_vma=False,
    )
```

```python
import functools

import jax
import jax.numpy as jnp
from jax import lax
from jax.experimental import pallas as pl
from jax.experimental.pallas import tpu as pltpu
from jax.sharding import PartitionSpec as P


HEADDIM = 64
NSTATE = 128
BLOCK = 128
LANES = 128
HALO = 8
PHASES = 2
PAD_ROWS = 16

HIGHEST = lax.Precision.HIGHEST
EPSILON = 1e-05
F32 = jnp.float32
BF16 = jnp.bfloat16


def cost(flops, bytes_accessed):
    return pl.CostEstimate(flops=int(flops), bytes_accessed=int(bytes_accessed), transcendentals=0)


def params(*semantics):
    return pltpu.CompilerParams(dimension_semantics=semantics, vmem_limit_bytes=48 * 1024 * 1024)


def silu(x):
    return x / (1.0 + jnp.exp(-x))


def dot(a, b, dims=(((1,), (0,)), ((), ()))):
    return lax.dot_general(a, b, dims, preferred_element_type=F32)


def spread(columns, pair):
    rows = columns.shape[0]
    lane = lax.broadcasted_iota(jnp.int32, (rows, LANES), 1)
    first = jnp.broadcast_to(columns[:, 2 * pair : 2 * pair + 1], (rows, LANES))
    second = jnp.broadcast_to(columns[:, 2 * pair + 1 : 2 * pair + 2], (rows, LANES))
    return jnp.where(lane < HEADDIM, first, second)


def mixer_local_kernel(
    values_ref,
    maps_ref,
    before_ref,
    step_ref,
    increment_ref,
    bias_ref,
    rate_ref,
    direct_ref,
    value_taps_ref,
    map_taps_ref,
    y_ref,
    out_maps_ref,
    prefix_ref,
    end_ref,
    extended,
    state,
    total,
):
    block = pl.program_id(0)
    channels = values_ref.shape[1]
    width = maps_ref.shape[2]
    groups = width // NSTATE
    heads = step_ref.shape[1]
    per_group = heads // groups
    group_lanes = per_group * HEADDIM
    taps = value_taps_ref.shape[0]

    @pl.when(block == 0)
    def _():
        extended[0:HALO, :] = before_ref[...].astype(F32)
        state[...] = jnp.zeros_like(state)
        total[...] = jnp.zeros_like(total)

    extended[HALO:, 0:channels] = values_ref[...].astype(F32)
    extended[HALO:, channels : channels + width] = maps_ref[0].astype(F32)
    extended[HALO:, channels + width :] = maps_ref[1].astype(F32)

    def conv(start, stop, weights):
        summed = jnp.zeros((BLOCK, stop - start), F32)
        for j in range(taps):
            at = HALO - (taps - 1) + j
            summed = summed + weights[j : j + 1, :] * extended[at : at + BLOCK, start:stop]
        return silu(summed)

    step = jax.nn.softplus(step_ref[...] + bias_ref[...])
    log_decay = step * rate_ref[...] + increment_ref[...]
    row = lax.broadcasted_iota(jnp.int32, (BLOCK, BLOCK), 0)
    column = lax.broadcasted_iota(jnp.int32, (BLOCK, BLOCK), 1)
    causal = row >= column
    running = lax.dot_general(
        causal.astype(F32),
        log_decay,
        (((1,), (0,)), ((), ())),
        precision=HIGHEST,
        preferred_element_type=F32,
    )
    running_rows = jnp.transpose(running)
    block_total = running[BLOCK - 1 : BLOCK, :]
    decay_in = jnp.exp(running)
    to_end = jnp.exp(block_total - running)
    prefix_ref[...] = jnp.exp(running + total[...])
    total[...] = total[...] + block_total
    block_decay = jnp.exp(block_total)

    for g in range(groups):
        in_map = conv(
            channels + g * NSTATE, channels + (g + 1) * NSTATE, map_taps_ref[0, :, g * NSTATE : (g + 1) * NSTATE].astype(F32)
        ).astype(BF16)
        out_map = conv(
            channels + width + g * NSTATE,
            channels + width + (g + 1) * NSTATE,
            map_taps_ref[1, :, g * NSTATE : (g + 1) * NSTATE].astype(F32),
        ).astype(BF16)
        out_maps_ref[:, g * NSTATE : (g + 1) * NSTATE] = out_map
        scores = dot(out_map, in_map, (((1,), (1,)), ((), ())))
        scores = jnp.where(causal, scores, 0.0)
        for pair in range(per_group // 2):
            first = g * (per_group // 2) + pair
            lanes = slice(first * LANES, (first + 1) * LANES)
            inner = slice(pair * LANES, (pair + 1) * LANES)
            x = conv(lanes.start, lanes.stop, value_taps_ref[:, lanes].astype(F32))
            scaled = x * spread(step, first)
            scaled_low = scaled.astype(BF16)
            parts = []
            for h in (2 * first, 2 * first + 1):
                gap = running[:, h : h + 1] - running_rows[h : h + 1, :]
                weights = scores * jnp.exp(jnp.minimum(gap, 0.0))
                parts.append(dot(weights.astype(BF16), scaled_low))
            lane = lax.broadcasted_iota(jnp.int32, (BLOCK, LANES), 1)
            inside = jnp.where(lane < HEADDIM, parts[0], parts[1])
            entering = state[g, :, inner]
            carried = dot(out_map, entering.astype(BF16)) * spread(decay_in, first)
            y_ref[:, lanes] = inside + carried + x * spread(direct_ref[...], first)
            ending = (scaled * spread(to_end, first)).astype(BF16)
            added = dot(in_map, ending, (((0,), (0,)), ((), ())))
            state[g, :, inner] = entering * spread(block_decay, first) + added

    extended[0:HALO, :] = extended[BLOCK : BLOCK + HALO, :]

    @pl.when(block == pl.num_programs(0) - 1)
    def _():
        end_ref[0 : groups * NSTATE, :] = (
            state[...].reshape(groups * NSTATE, group_lanes).astype(BF16)
        )
        total_decay = jnp.exp(total[...])
        row_at = lax.broadcasted_iota(jnp.int32, (PAD_ROWS, LANES), 0)
        for pair in range(per_group // 2):
            decays = jnp.zeros((PAD_ROWS, LANES), F32)
            for g in range(groups):
                decay = spread(total_decay, g * (per_group // 2) + pair)
                decays = jnp.where(row_at == g, decay, decays)
            end_ref[groups * NSTATE :, pair * LANES : (pair + 1) * LANES] = decays.astype(BF16)


def merge_kernel(earlier_ref, later_ref, out_ref):
    split = later_ref.shape[0] - PAD_ROWS
    decays = later_ref[split:, :].astype(F32)
    for g in range(split // NSTATE):
        rows = slice(g * NSTATE, (g + 1) * NSTATE)
        merged = later_ref[rows, :].astype(F32) + decays[g : g + 1, :] * earlier_ref[
            rows, :
        ].astype(F32)
        out_ref[rows, :] = merged.astype(BF16)
    out_ref[split:, :] = (decays * earlier_ref[split:, :].astype(F32)).astype(BF16)


def mixer_finish_kernel(y_ref, out_maps_ref, prefix_ref, incoming_ref, gate_ref, gain_ref, out_ref):
    heads = prefix_ref.shape[1]
    groups = out_maps_ref.shape[1] // NSTATE
    per_group = heads // groups
    prefix = prefix_ref[...]
    for g in range(groups):
        out_map = out_maps_ref[:, g * NSTATE : (g + 1) * NSTATE]
        parts = []
        squares = 0.0
        for pair in range(per_group // 2):
            first = g * (per_group // 2) + pair
            lanes = slice(first * LANES, (first + 1) * LANES)
            incoming = incoming_ref[
                g * NSTATE : (g + 1) * NSTATE, pair * LANES : (pair + 1) * LANES
            ]
            y = y_ref[:, lanes] + dot(out_map, incoming) * spread(prefix, first)
            gated = y * silu(gate_ref[:, lanes].astype(F32))
            squares = squares + jnp.sum(gated * gated, axis=1, keepdims=True)
            parts.append((lanes, gated))
        scale = lax.rsqrt(squares / (per_group * HEADDIM) + EPSILON)
        for lanes, gated in parts:
            out_ref[:, lanes] = (gated * scale * gain_ref[:, lanes]).astype(BF16)


def dispatch_kernel(tokens_ref, gain_ref, routes_ref, *refs, capacity):
    target_ref = refs[-1]
    tokens = tokens_ref.shape[0]
    rows = refs[0].shape[0] * PHASES
    part = capacity // PHASES
    values = tokens_ref[...].astype(F32)
    centered = values - jnp.mean(values, axis=1, keepdims=True)
    variance = jnp.mean(centered * centered, axis=1, keepdims=True)
    normed = (centered * lax.rsqrt(variance + EPSILON) * gain_ref[...]).astype(BF16)
    routes = routes_ref[...]
    fanout = routes.shape[1]
    experts = lax.broadcasted_iota(jnp.int32, (tokens, LANES), 1)
    visits = jnp.zeros((tokens, LANES), F32)
    for k in range(fanout):
        visits = visits + (experts == routes[:, k : k + 1]).astype(F32)
    row = lax.broadcasted_iota(jnp.int32, (tokens, tokens), 0)
    column = lax.broadcasted_iota(jnp.int32, (tokens, tokens), 1)
    slots = dot((row > column).astype(F32).astype(BF16), visits.astype(BF16)).astype(jnp.int32)
    phase = jnp.zeros_like(slots)
    for late in range(1, PHASES):
        phase = phase + (slots >= late * part).astype(jnp.int32)
    slots = slots + phase * (rows // PHASES - part) + experts * part
    places = lax.broadcasted_iota(jnp.int32, (tokens, rows), 1)
    chosen = jnp.zeros((tokens, rows), F32)
    for k in range(fanout):
        target = jnp.sum(
            jnp.where(experts == routes[:, k : k + 1], slots.astype(F32), 0.0), axis=1, keepdims=True
        ).astype(jnp.int32)
        target_ref[:, k : k + 1] = target
        chosen = chosen + (places == target).astype(F32)
    chosen = chosen.astype(BF16)
    size = rows // PHASES
    for at, rows_ref in enumerate(refs[:-1]):
        picked = chosen[:, at * size : (at + 1) * size]
        rows_ref[...] = dot(picked, normed, (((0,), (0,)), ((), ()))).astype(BF16)


def combine_kernel(*refs, offset):
    returned_ref, target_ref, weight_ref = refs[:3]
    out_ref = refs[-1]
    tokens = target_ref.shape[0]
    rows = returned_ref.shape[0]
    places = lax.broadcasted_iota(jnp.int32, (tokens, rows), 1) + offset
    table = jnp.zeros((tokens, rows), F32)
    for k in range(target_ref.shape[1]):
        table = table + jnp.where(places == target_ref[:, k : k + 1], weight_ref[:, k : k + 1], 0.0)
    high = table.astype(BF16)
    low = (table - high.astype(F32)).astype(BF16)
    returned = returned_ref[...]
    summed = dot(high, returned) + dot(low, returned)
    if len(refs) > 4:
        summed = summed + refs[3][...]
    out_ref[...] = summed.astype(out_ref.dtype)


def hidden_kernel(*refs):
    rows_ref, hidden_ref = refs[0], refs[-1]
    count = (len(refs) - 2) // 2
    units = refs[1].shape[2]
    for at in range(count):
        rows = rows_ref[...]
        activated = silu(dot(rows, refs[1 + at][0]))
        hidden_ref[:, at * units : (at + 1) * units] = (
            activated * dot(rows, refs[1 + count + at][0])
        ).astype(BF16)


def down_kernel(*refs):
    hidden_ref, out_ref = refs[0], refs[-1]
    units = refs[1].shape[2]
    total = 0.0
    for at, down_ref in enumerate(refs[1:-1]):
        hidden = hidden_ref[:, at * units : (at + 1) * units]
        total = total + dot(hidden, down_ref[0], (((1,), (1,)), ((), ())))
    out_ref[...] = total.astype(BF16)


def whole(shape):
    return pl.BlockSpec(shape, lambda *_: (0,) * len(shape))


def shifted(block, axis, distance):
    devices = range(lax.axis_size(axis))
    route = [(i - distance, i) for i in devices if i - distance in devices]
    return lax.ppermute(block, axis, route)


def flipped(block, axis, bit):
    return lax.ppermute(block, axis, [(i, i ^ bit) for i in range(lax.axis_size(axis))])


def all_shards(block, axis):
    pieces = [block]
    bit = lax.axis_size(axis) // 2
    while bit:
        moved = []
        for piece in pieces:
            moved.append(flipped(piece, axis, bit))
        pieces = pieces + moved
        bit //= 2
    return pieces


def mixer_local(
    values,
    maps,
    before,
    step_preactivation,
    step_bias,
    log_rate,
    increment,
    direct,
    value_taps,
    map_taps,
):
    length, channels = values.shape
    heads = step_preactivation.shape[1]
    width = maps.shape[2]
    groups = width // NSTATE
    group_lanes = channels // groups
    taps = value_taps.shape[0]
    return pl.pallas_call(
        mixer_local_kernel,
        grid=(length // BLOCK,),
        in_specs=[
            pl.BlockSpec((BLOCK, channels), lambda i: (i, 0)),
            pl.BlockSpec((2, BLOCK, width), lambda i: (0, i, 0)),
            whole((HALO, channels + 2 * width)),
            pl.BlockSpec((BLOCK, heads), lambda i: (i, 0)),
            pl.BlockSpec((BLOCK, heads), lambda i: (i, 0)),
            whole((1, heads)),
            whole((1, heads)),
            whole((1, heads)),
            whole((taps, channels)),
            whole((2, taps, width)),
        ],
        out_specs=[
            pl.BlockSpec((BLOCK, channels), lambda i: (i, 0)),
            pl.BlockSpec((BLOCK, width), lambda i: (i, 0)),
            pl.BlockSpec((BLOCK, heads), lambda i: (i, 0)),
            whole((groups * NSTATE + PAD_ROWS, group_lanes)),
        ],
        out_shape=[
            jax.ShapeDtypeStruct((length, channels), F32),
            jax.ShapeDtypeStruct((length, width), BF16),
            jax.ShapeDtypeStruct((length, heads), F32),
            jax.ShapeDtypeStruct((groups * NSTATE + PAD_ROWS, group_lanes), BF16),
        ],
        scratch_shapes=[
            pltpu.VMEM((BLOCK + HALO, channels + 2 * width), F32),
            pltpu.VMEM((groups, NSTATE, group_lanes), F32),
            pltpu.VMEM((1, heads), F32),
        ],
        compiler_params=params("arbitrary"),
        cost_estimate=cost(15e9, 8e6),
        name="mixer_local",
    )(
        values,
        maps,
        before,
        step_preactivation,
        increment,
        step_bias[None],
        -jnp.exp(log_rate)[None],
        direct[None],
        value_taps,
        map_taps,
    )


def merged_states(earlier, later):
    return pl.pallas_call(
        merge_kernel,
        out_shape=jax.ShapeDtypeStruct(later.shape, later.dtype),
        compiler_params=params(),
        cost_estimate=cost(1e6, 4e5),
        name="merge",
    )(earlier, later)


def incoming_state(end):
    carried = shifted(end, "ep", 1)
    distance = 1
    while distance < lax.axis_size("ep") - 1:
        earlier = shifted(carried, "ep", distance)
        carried = merged_states(earlier, carried)
        distance *= 2
    return carried


def mixer_finish(y, out_maps, prefix, incoming, gate, gain):
    length, channels = y.shape
    tile = min(256, length)
    width = out_maps.shape[1]
    return pl.pallas_call(
        mixer_finish_kernel,
        grid=(length // tile,),
        in_specs=[
            pl.BlockSpec((tile, channels), lambda i: (i, 0)),
            pl.BlockSpec((tile, width), lambda i: (i, 0)),
            pl.BlockSpec((tile, prefix.shape[1]), lambda i: (i, 0)),
            whole(incoming.shape),
            pl.BlockSpec((tile, channels), lambda i: (i, 0)),
            whole((1, channels)),
        ],
        out_specs=pl.BlockSpec((tile, channels), lambda i: (i, 0)),
        out_shape=jax.ShapeDtypeStruct((length, channels), BF16),
        compiler_params=params("arbitrary"),
        cost_estimate=cost(4e9, 8e6),
        name="mixer_finish",
    )(y, out_maps, prefix, incoming, gate, gain[None])


def dispatched(tokens, gain, routes, rows, capacity):
    _, features = tokens.shape
    return pl.pallas_call(
        functools.partial(dispatch_kernel, capacity=capacity),
        out_shape=[
            *[jax.ShapeDtypeStruct((rows // PHASES, features), BF16)] * PHASES,
            jax.ShapeDtypeStruct(routes.shape, jnp.int32),
        ],
        compiler_params=params(),
        cost_estimate=cost(2e9, 5e6),
        name="dispatch",
    )(tokens, gain[None], routes)


def hidden_units(rows, gates, ups):
    count, features = rows.shape
    units = gates[0].shape[2] * len(gates)
    return pl.pallas_call(
        hidden_kernel,
        out_shape=jax.ShapeDtypeStruct((count, units), BF16),
        compiler_params=params(),
        cost_estimate=cost(4 * count * features * units, 1e7),
        name="hidden",
    )(rows, *gates, *ups)


def projected(hidden, downs):
    count, units = hidden.shape
    features, piece = downs[0].shape[1:]
    tile = min(512, features)
    return pl.pallas_call(
        down_kernel,
        grid=(features // tile,),
        in_specs=[whole(hidden.shape)]
        + [pl.BlockSpec((1, tile, piece), lambda i: (0, i, 0)) for d in downs],
        out_specs=pl.BlockSpec((count, tile), lambda i: (0, i)),
        out_shape=jax.ShapeDtypeStruct((count, features), BF16),
        compiler_params=params("arbitrary"),
        cost_estimate=cost(2 * count * features * units, 5e6),
        name="down",
    )(hidden, *downs)


def combined_rows(returned, target, weight, offset, partial, dtype):
    rows, features = returned.shape
    tile = min(512, features)
    tiles = pl.BlockSpec((target.shape[0], tile), lambda i: (0, i))
    partial = [] if partial is None else [partial]
    return pl.pallas_call(
        functools.partial(combine_kernel, offset=offset),
        grid=(features // tile,),
        in_specs=[
            pl.BlockSpec((rows, tile), lambda i: (0, i)),
            whole(target.shape),
            whole(weight.shape),
        ]
        + [tiles] * len(partial),
        out_specs=tiles,
        out_shape=jax.ShapeDtypeStruct((target.shape[0], features), dtype),
        compiler_params=params("arbitrary"),
        cost_estimate=cost(2e9, 4e6),
        name="combine",
    )(returned, target, weight, *partial)


def exchanged(rows, experts):
    count, features = rows.shape
    swapped = lax.all_to_all(
        rows.reshape(experts, count // experts, features),
        "ep",
        split_axis=0,
        concat_axis=0,
        tiled=True,
    )
    return swapped.reshape(count, features)


def body(
    first_micro_values,
    group_state_maps,
    gate_preactivation,
    step_preactivation,
    head_step_bias,
    head_log_decay,
    decay_increment,
    head_direct_gain,
    convolution_value_taps,
    convolution_map_taps,
    grouped_norm_gain,
    second_micro_tokens,
    expert_norm_gain,
    routes,
    visit_weight,
    gate_weight_table,
    up_weight_table,
    down_weight_table,
):
    tokens, _ = second_micro_tokens.shape
    length = first_micro_values.shape[0]
    experts = lax.axis_size("ep")
    capacity = max(2, 3 * tokens * routes.shape[1] // (2 * experts))
    size = experts * capacity // PHASES
    tail_rows = jnp.concatenate(
        [
            first_micro_values[length - HALO :],
            group_state_maps[0, length - HALO :],
            group_state_maps[1, length - HALO :],
        ],
        axis=1,
    )
    gates = all_shards(gate_weight_table, "tp")
    ups = all_shards(up_weight_table, "tp")
    downs = all_shards(down_weight_table, "tp")
    before = shifted(tail_rows, "ep", 1)
    *outgoing, target = dispatched(
        second_micro_tokens, expert_norm_gain, routes, experts * capacity, capacity
    )
    arrived = []
    for rows in outgoing:
        arrived.append(exchanged(rows, experts))
    y, out_maps, prefix, end = mixer_local(
        first_micro_values,
        group_state_maps,
        before,
        step_preactivation,
        head_step_bias,
        head_log_decay,
        decay_increment,
        head_direct_gain,
        convolution_value_taps,
        convolution_map_taps,
    )
    incoming = incoming_state(end)
    total = None
    for at, rows in enumerate(arrived):
        hidden = hidden_units(rows, gates, ups)
        results = projected(hidden, downs)
        returned = exchanged(results, experts)
        dtype = BF16 if at + 1 == PHASES else F32
        total = combined_rows(returned, target, visit_weight, at * size, total, dtype)
    mixer_out = mixer_finish(
        y, out_maps, prefix, incoming, gate_preactivation, grouped_norm_gain
    )
    return (mixer_out, total)


def solution(mesh):
    placed = (
        P("ep", "tp"),
        P(None, "ep", "tp"),
        P("ep", "tp"),
        P("ep", "tp"),
        P("tp"),
        P("tp"),
        P("ep", "tp"),
        P("tp"),
        P(None, "tp"),
        P(None, None, "tp"),
        P("tp"),
        P(("ep", "tp"), None),
        P(),
        P(("ep", "tp"), None),
        P(("ep", "tp"), None),
        P("ep", None, "tp"),
        P("ep", None, "tp"),
        P("ep", None, "tp"),
    )
    return jax.shard_map(
        body,
        mesh=mesh,
        in_specs=placed,
        out_specs=(P("ep", "tp"), P(("ep", "tp"), None)),
        check_vma=False,
    )
```

```python
import functools

import jax
import jax.numpy as jnp
from jax import lax
from jax.experimental import pallas as pl
from jax.experimental.pallas import tpu as pltpu
from jax.sharding import PartitionSpec as P


HEADDIM = 64
NSTATE = 128
BLOCK = 128
LANES = 128
HALO = 8
PHASES = 2
PAD_ROWS = 16

HIGHEST = lax.Precision.HIGHEST
EPSILON = 1e-05
F32 = jnp.float32
BF16 = jnp.bfloat16


def cost(flops, bytes_accessed):
    return pl.CostEstimate(flops=int(flops), bytes_accessed=int(bytes_accessed), transcendentals=0)


def params(*semantics):
    return pltpu.CompilerParams(dimension_semantics=semantics, vmem_limit_bytes=62 * 1024 * 1024)


def silu(x):
    return x / (1.0 + jnp.exp(-x))


def dot(a, b, dims=(((1,), (0,)), ((), ()))):
    return lax.dot_general(a, b, dims, preferred_element_type=F32)


def spread(columns, pair):
    rows = columns.shape[0]
    lane = lax.broadcasted_iota(jnp.int32, (rows, LANES), 1)
    first = jnp.broadcast_to(columns[:, 2 * pair : 2 * pair + 1], (rows, LANES))
    second = jnp.broadcast_to(columns[:, 2 * pair + 1 : 2 * pair + 2], (rows, LANES))
    return jnp.where(lane < HEADDIM, first, second)


def mixer_local_kernel(
    values_ref,
    maps_ref,
    before_ref,
    step_ref,
    increment_ref,
    bias_ref,
    rate_ref,
    direct_ref,
    value_taps_ref,
    map_taps_ref,
    y_ref,
    out_maps_ref,
    prefix_ref,
    end_ref,
    extended,
    state,
    total,
):
    block = pl.program_id(0)
    channels = values_ref.shape[1]
    width = maps_ref.shape[2]
    groups = width // NSTATE
    heads = step_ref.shape[1]
    per_group = heads // groups
    group_lanes = per_group * HEADDIM
    taps = value_taps_ref.shape[0]

    @pl.when(block == 0)
    def _():
        extended[0:HALO, :] = before_ref[...].astype(F32)
        state[...] = jnp.zeros_like(state)
        total[...] = jnp.zeros_like(total)

    extended[HALO:, 0:channels] = values_ref[...].astype(F32)
    extended[HALO:, channels : channels + width] = maps_ref[0].astype(F32)
    extended[HALO:, channels + width :] = maps_ref[1].astype(F32)

    def conv(start, stop, weights):
        summed = jnp.zeros((BLOCK, stop - start), F32)
        for j in range(taps):
            at = HALO - (taps - 1) + j
            summed = summed + weights[j : j + 1, :] * extended[at : at + BLOCK, start:stop]
        return silu(summed)

    step = jax.nn.softplus(step_ref[...] + bias_ref[...])
    log_decay = step * rate_ref[...] + increment_ref[...]
    row = lax.broadcasted_iota(jnp.int32, (BLOCK, BLOCK), 0)
    column = lax.broadcasted_iota(jnp.int32, (BLOCK, BLOCK), 1)
    causal = row >= column
    running = lax.dot_general(
        causal.astype(F32),
        log_decay,
        (((1,), (0,)), ((), ())),
        precision=HIGHEST,
        preferred_element_type=F32,
    )
    running_rows = jnp.transpose(running)
    block_total = running[BLOCK - 1 : BLOCK, :]
    decay_in = jnp.exp(running)
    to_end = jnp.exp(block_total - running)
    prefix_ref[...] = jnp.exp(running + total[...])
    total[...] = total[...] + block_total
    block_decay = jnp.exp(block_total)

    for g in range(groups):
        in_map = conv(
            channels + g * NSTATE, channels + (g + 1) * NSTATE, map_taps_ref[0, :, g * NSTATE : (g + 1) * NSTATE].astype(F32)
        ).astype(BF16)
        out_map = conv(
            channels + width + g * NSTATE,
            channels + width + (g + 1) * NSTATE,
            map_taps_ref[1, :, g * NSTATE : (g + 1) * NSTATE].astype(F32),
        ).astype(BF16)
        out_maps_ref[:, g * NSTATE : (g + 1) * NSTATE] = out_map
        scores = dot(out_map, in_map, (((1,), (1,)), ((), ())))
        scores = jnp.where(causal, scores, 0.0)
        for pair in range(per_group // 2):
            first = g * (per_group // 2) + pair
            lanes = slice(first * LANES, (first + 1) * LANES)
            inner = slice(pair * LANES, (pair + 1) * LANES)
            x = conv(lanes.start, lanes.stop, value_taps_ref[:, lanes].astype(F32))
            scaled = x * spread(step, first)
            scaled_low = scaled.astype(BF16)
            parts = []
            for h in (2 * first, 2 * first + 1):
                gap = running[:, h : h + 1] - running_rows[h : h + 1, :]
                weights = scores * jnp.exp(jnp.minimum(gap, 0.0))
                parts.append(dot(weights.astype(BF16), scaled_low))
            lane = lax.broadcasted_iota(jnp.int32, (BLOCK, LANES), 1)
            inside = jnp.where(lane < HEADDIM, parts[0], parts[1])
            entering = state[g, :, inner]
            carried = dot(out_map, entering.astype(BF16)) * spread(decay_in, first)
            y_ref[:, lanes] = inside + carried + x * spread(direct_ref[...], first)
            ending = (scaled * spread(to_end, first)).astype(BF16)
            added = dot(in_map, ending, (((0,), (0,)), ((), ())))
            state[g, :, inner] = entering * spread(block_decay, first) + added

    extended[0:HALO, :] = extended[BLOCK : BLOCK + HALO, :]

    @pl.when(block == pl.num_programs(0) - 1)
    def _():
        end_ref[0 : groups * NSTATE, :] = (
            state[...].reshape(groups * NSTATE, group_lanes).astype(BF16)
        )
        total_decay = jnp.exp(total[...])
        row_at = lax.broadcasted_iota(jnp.int32, (PAD_ROWS, LANES), 0)
        for pair in range(per_group // 2):
            decays = jnp.zeros((PAD_ROWS, LANES), F32)
            for g in range(groups):
                decay = spread(total_decay, g * (per_group // 2) + pair)
                decays = jnp.where(row_at == g, decay, decays)
            end_ref[groups * NSTATE :, pair * LANES : (pair + 1) * LANES] = decays.astype(BF16)


def merge_kernel(earlier_ref, later_ref, out_ref):
    split = later_ref.shape[0] - PAD_ROWS
    decays = later_ref[split:, :].astype(F32)
    for g in range(split // NSTATE):
        rows = slice(g * NSTATE, (g + 1) * NSTATE)
        merged = later_ref[rows, :].astype(F32) + decays[g : g + 1, :] * earlier_ref[
            rows, :
        ].astype(F32)
        out_ref[rows, :] = merged.astype(BF16)
    out_ref[split:, :] = (decays * earlier_ref[split:, :].astype(F32)).astype(BF16)


def mixer_finish_kernel(y_ref, out_maps_ref, prefix_ref, incoming_ref, gate_ref, gain_ref, out_ref):
    heads = prefix_ref.shape[1]
    groups = out_maps_ref.shape[1] // NSTATE
    per_group = heads // groups
    prefix = prefix_ref[...]
    for g in range(groups):
        out_map = out_maps_ref[:, g * NSTATE : (g + 1) * NSTATE]
        parts = []
        squares = 0.0
        for pair in range(per_group // 2):
            first = g * (per_group // 2) + pair
            lanes = slice(first * LANES, (first + 1) * LANES)
            incoming = incoming_ref[
                g * NSTATE : (g + 1) * NSTATE, pair * LANES : (pair + 1) * LANES
            ]
            y = y_ref[:, lanes] + dot(out_map, incoming) * spread(prefix, first)
            gated = y * silu(gate_ref[:, lanes].astype(F32))
            squares = squares + jnp.sum(gated * gated, axis=1, keepdims=True)
            parts.append((lanes, gated))
        scale = lax.rsqrt(squares / (per_group * HEADDIM) + EPSILON)
        for lanes, gated in parts:
            out_ref[:, lanes] = (gated * scale * gain_ref[:, lanes]).astype(BF16)


def dispatch_kernel(tokens_ref, gain_ref, routes_ref, *refs, capacity):
    target_ref = refs[-1]
    tokens = tokens_ref.shape[0]
    rows = refs[0].shape[0] * PHASES
    part = capacity // PHASES
    values = tokens_ref[...].astype(F32)
    centered = values - jnp.mean(values, axis=1, keepdims=True)
    variance = jnp.mean(centered * centered, axis=1, keepdims=True)
    normed = (centered * lax.rsqrt(variance + EPSILON) * gain_ref[...]).astype(BF16)
    routes = routes_ref[...]
    fanout = routes.shape[1]
    experts = lax.broadcasted_iota(jnp.int32, (tokens, LANES), 1)
    visits = jnp.zeros((tokens, LANES), F32)
    for k in range(fanout):
        visits = visits + (experts == routes[:, k : k + 1]).astype(F32)
    row = lax.broadcasted_iota(jnp.int32, (tokens, tokens), 0)
    column = lax.broadcasted_iota(jnp.int32, (tokens, tokens), 1)
    slots = dot((row > column).astype(F32).astype(BF16), visits.astype(BF16)).astype(jnp.int32)
    phase = jnp.zeros_like(slots)
    for late in range(1, PHASES):
        phase = phase + (slots >= late * part).astype(jnp.int32)
    slots = slots + phase * (rows // PHASES - part) + experts * part
    places = lax.broadcasted_iota(jnp.int32, (tokens, rows), 1)
    chosen = jnp.zeros((tokens, rows), F32)
    for k in range(fanout):
        target = jnp.sum(
            jnp.where(experts == routes[:, k : k + 1], slots.astype(F32), 0.0), axis=1, keepdims=True
        ).astype(jnp.int32)
        target_ref[:, k : k + 1] = target
        chosen = chosen + (places == target).astype(F32)
    chosen = chosen.astype(BF16)
    size = rows // PHASES
    for at, rows_ref in enumerate(refs[:-1]):
        picked = chosen[:, at * size : (at + 1) * size]
        rows_ref[...] = dot(picked, normed, (((0,), (0,)), ((), ()))).astype(BF16)


def combine_kernel(*refs, offset):
    returned_ref, target_ref, weight_ref = refs[:3]
    out_ref = refs[-1]
    tokens = target_ref.shape[0]
    rows = returned_ref.shape[0]
    places = lax.broadcasted_iota(jnp.int32, (tokens, rows), 1) + offset
    table = jnp.zeros((tokens, rows), F32)
    for k in range(target_ref.shape[1]):
        table = table + jnp.where(places == target_ref[:, k : k + 1], weight_ref[:, k : k + 1], 0.0)
    high = table.astype(BF16)
    low = (table - high.astype(F32)).astype(BF16)
    returned = returned_ref[...]
    summed = dot(high, returned) + dot(low, returned)
    if len(refs) > 4:
        summed = summed + refs[3][...]
    out_ref[...] = summed.astype(out_ref.dtype)


def hidden_kernel(*refs):
    rows_ref, hidden_ref = refs[0], refs[-1]
    count = (len(refs) - 2) // 2
    units = refs[1].shape[2]
    for at in range(count):
        rows = rows_ref[...]
        activated = silu(dot(rows, refs[1 + at][0]))
        hidden_ref[:, at * units : (at + 1) * units] = (
            activated * dot(rows, refs[1 + count + at][0])
        ).astype(BF16)


def down_kernel(*refs):
    hidden_ref, out_ref = refs[0], refs[-1]
    units = refs[1].shape[2]
    total = 0.0
    for at, down_ref in enumerate(refs[1:-1]):
        hidden = hidden_ref[:, at * units : (at + 1) * units]
        total = total + dot(hidden, down_ref[0], (((1,), (1,)), ((), ())))
    out_ref[...] = total.astype(BF16)


def whole(shape):
    return pl.BlockSpec(shape, lambda *_: (0,) * len(shape))


def shifted(block, axis, distance):
    devices = range(lax.axis_size(axis))
    route = [(i - distance, i) for i in devices if i - distance in devices]
    return lax.ppermute(block, axis, route)


def flipped(block, axis, bit):
    return lax.ppermute(block, axis, [(i, i ^ bit) for i in range(lax.axis_size(axis))])


def all_shards(block, axis):
    pieces = [block]
    bit = lax.axis_size(axis) // 2
    while bit:
        moved = []
        for piece in pieces:
            moved.append(flipped(piece, axis, bit))
        pieces = pieces + moved
        bit //= 2
    return pieces


def mixer_local(
    values,
    maps,
    before,
    step_preactivation,
    step_bias,
    log_rate,
    increment,
    direct,
    value_taps,
    map_taps,
):
    length, channels = values.shape
    heads = step_preactivation.shape[1]
    width = maps.shape[2]
    groups = width // NSTATE
    group_lanes = channels // groups
    taps = value_taps.shape[0]
    return pl.pallas_call(
        mixer_local_kernel,
        grid=(length // BLOCK,),
        in_specs=[
            pl.BlockSpec((BLOCK, channels), lambda i: (i, 0)),
            pl.BlockSpec((2, BLOCK, width), lambda i: (0, i, 0)),
            whole((HALO, channels + 2 * width)),
            pl.BlockSpec((BLOCK, heads), lambda i: (i, 0)),
            pl.BlockSpec((BLOCK, heads), lambda i: (i, 0)),
            whole((1, heads)),
            whole((1, heads)),
            whole((1, heads)),
            whole((taps, channels)),
            whole((2, taps, width)),
        ],
        out_specs=[
            pl.BlockSpec((BLOCK, channels), lambda i: (i, 0)),
            pl.BlockSpec((BLOCK, width), lambda i: (i, 0)),
            pl.BlockSpec((BLOCK, heads), lambda i: (i, 0)),
            whole((groups * NSTATE + PAD_ROWS, group_lanes)),
        ],
        out_shape=[
            jax.ShapeDtypeStruct((length, channels), F32),
            jax.ShapeDtypeStruct((length, width), BF16),
            jax.ShapeDtypeStruct((length, heads), F32),
            jax.ShapeDtypeStruct((groups * NSTATE + PAD_ROWS, group_lanes), BF16),
        ],
        scratch_shapes=[
            pltpu.VMEM((BLOCK + HALO, channels + 2 * width), F32),
            pltpu.VMEM((groups, NSTATE, group_lanes), F32),
            pltpu.VMEM((1, heads), F32),
        ],
        compiler_params=params("arbitrary"),
        cost_estimate=cost(15e9, 8e6),
        name="mixer_local",
    )(
        values,
        maps,
        before,
        step_preactivation,
        increment,
        step_bias[None],
        -jnp.exp(log_rate)[None],
        direct[None],
        value_taps,
        map_taps,
    )


def merged_states(earlier, later):
    return pl.pallas_call(
        merge_kernel,
        out_shape=jax.ShapeDtypeStruct(later.shape, later.dtype),
        compiler_params=params(),
        cost_estimate=cost(1e6, 4e5),
        name="merge",
    )(earlier, later)


def incoming_state(end):
    nearest = shifted(end, "ep", 1)
    carried = merged_states(shifted(end, "ep", 2), nearest)
    distance = 2
    while distance < lax.axis_size("ep") - 1:
        carried = merged_states(shifted(carried, "ep", distance), carried)
        distance *= 2
    return carried


def mixer_finish(y, out_maps, prefix, incoming, gate, gain):
    length, channels = y.shape
    tile = min(256, length)
    width = out_maps.shape[1]
    return pl.pallas_call(
        mixer_finish_kernel,
        grid=(length // tile,),
        in_specs=[
            pl.BlockSpec((tile, channels), lambda i: (i, 0)),
            pl.BlockSpec((tile, width), lambda i: (i, 0)),
            pl.BlockSpec((tile, prefix.shape[1]), lambda i: (i, 0)),
            whole(incoming.shape),
            pl.BlockSpec((tile, channels), lambda i: (i, 0)),
            whole((1, channels)),
        ],
        out_specs=pl.BlockSpec((tile, channels), lambda i: (i, 0)),
        out_shape=jax.ShapeDtypeStruct((length, channels), BF16),
        compiler_params=params("arbitrary"),
        cost_estimate=cost(4e9, 8e6),
        name="mixer_finish",
    )(y, out_maps, prefix, incoming, gate, gain[None])


def dispatched(tokens, gain, routes, rows, capacity):
    _, features = tokens.shape
    return pl.pallas_call(
        functools.partial(dispatch_kernel, capacity=capacity),
        out_shape=[
            *[jax.ShapeDtypeStruct((rows // PHASES, features), BF16)] * PHASES,
            jax.ShapeDtypeStruct(routes.shape, jnp.int32),
        ],
        compiler_params=params(),
        cost_estimate=cost(2e9, 5e6),
        name="dispatch",
    )(tokens, gain[None], routes)


def hidden_units(rows, gates, ups):
    count, features = rows.shape
    units = gates[0].shape[2] * len(gates)
    return pl.pallas_call(
        hidden_kernel,
        out_shape=jax.ShapeDtypeStruct((count, units), BF16),
        compiler_params=params(),
        cost_estimate=cost(4 * count * features * units, 1e7),
        name="hidden",
    )(rows, *gates, *ups)


def projected(hidden, downs):
    count, units = hidden.shape
    features, piece = downs[0].shape[1:]
    tile = min(512, features)
    return pl.pallas_call(
        down_kernel,
        grid=(features // tile,),
        in_specs=[whole(hidden.shape)]
        + [pl.BlockSpec((1, tile, piece), lambda i: (0, i, 0)) for d in downs],
        out_specs=pl.BlockSpec((count, tile), lambda i: (0, i)),
        out_shape=jax.ShapeDtypeStruct((count, features), BF16),
        compiler_params=params("arbitrary"),
        cost_estimate=cost(2 * count * features * units, 5e6),
        name="down",
    )(hidden, *downs)


def combined_rows(returned, target, weight, offset, partial, dtype):
    rows, features = returned.shape
    tile = min(512, features)
    tiles = pl.BlockSpec((target.shape[0], tile), lambda i: (0, i))
    partial = [] if partial is None else [partial]
    return pl.pallas_call(
        functools.partial(combine_kernel, offset=offset),
        grid=(features // tile,),
        in_specs=[
            pl.BlockSpec((rows, tile), lambda i: (0, i)),
            whole(target.shape),
            whole(weight.shape),
        ]
        + [tiles] * len(partial),
        out_specs=tiles,
        out_shape=jax.ShapeDtypeStruct((target.shape[0], features), dtype),
        compiler_params=params("arbitrary"),
        cost_estimate=cost(2e9, 4e6),
        name="combine",
    )(returned, target, weight, *partial)


def exchanged(rows, experts):
    count, features = rows.shape
    swapped = lax.all_to_all(
        rows.reshape(experts, count // experts, features),
        "ep",
        split_axis=0,
        concat_axis=0,
        tiled=True,
    )
    return swapped.reshape(count, features)


def body(
    first_micro_values,
    group_state_maps,
    gate_preactivation,
    step_preactivation,
    head_step_bias,
    head_log_decay,
    decay_increment,
    head_direct_gain,
    convolution_value_taps,
    convolution_map_taps,
    grouped_norm_gain,
    second_micro_tokens,
    expert_norm_gain,
    routes,
    visit_weight,
    gate_weight_table,
    up_weight_table,
    down_weight_table,
):
    tokens, _ = second_micro_tokens.shape
    length = first_micro_values.shape[0]
    experts = lax.axis_size("ep")
    capacity = max(2, 3 * tokens * routes.shape[1] // (2 * experts))
    size = experts * capacity // PHASES
    tail_rows = jnp.concatenate(
        [
            first_micro_values[length - HALO :],
            group_state_maps[0, length - HALO :],
            group_state_maps[1, length - HALO :],
        ],
        axis=1,
    )
    gates = all_shards(gate_weight_table, "tp")
    ups = all_shards(up_weight_table, "tp")
    downs = all_shards(down_weight_table, "tp")
    before = shifted(tail_rows, "ep", 1)
    *outgoing, target = dispatched(
        second_micro_tokens, expert_norm_gain, routes, experts * capacity, capacity
    )
    arrived = []
    for rows in outgoing:
        arrived.append(exchanged(rows, experts))
    y, out_maps, prefix, end = mixer_local(
        first_micro_values,
        group_state_maps,
        before,
        step_preactivation,
        head_step_bias,
        head_log_decay,
        decay_increment,
        head_direct_gain,
        convolution_value_taps,
        convolution_map_taps,
    )
    incoming = incoming_state(end)
    total = None
    for at, rows in enumerate(arrived):
        hidden = hidden_units(rows, gates, ups)
        results = projected(hidden, downs)
        returned = exchanged(results, experts)
        dtype = BF16 if at + 1 == PHASES else F32
        total = combined_rows(returned, target, visit_weight, at * size, total, dtype)
    mixer_out = mixer_finish(
        y, out_maps, prefix, incoming, gate_preactivation, grouped_norm_gain
    )
    return (mixer_out, total)


def solution(mesh):
    placed = (
        P("ep", "tp"),
        P(None, "ep", "tp"),
        P("ep", "tp"),
        P("ep", "tp"),
        P("tp"),
        P("tp"),
        P("ep", "tp"),
        P("tp"),
        P(None, "tp"),
        P(None, None, "tp"),
        P("tp"),
        P(("ep", "tp"), None),
        P(),
        P(("ep", "tp"), None),
        P(("ep", "tp"), None),
        P("ep", None, "tp"),
        P("ep", None, "tp"),
        P("ep", None, "tp"),
    )
    return jax.shard_map(
        body,
        mesh=mesh,
        in_specs=placed,
        out_specs=(P("ep", "tp"), P(("ep", "tp"), None)),
        check_vma=False,
    )
```
